32 devices in a mesh: fs: 4 (over y, x), tp: 8 (over z, core).
Axes of the slice: x: 2, y: 2, z: 4, core: 2. Of those that a mesh axis runs over, the one named last changes fastest.
Arguments:
- value_input: bfloat16 [8192, 2048], P('fs', 'tp'), may hold values from -50 to 50
- value_cotangent: bfloat16 [8192, 512], P('fs'), may hold values from -6 to 6
- value_factor: bfloat16 [512, 128], replicated, may hold values from -10 to 10
- value_master: float32 [512, 2048], P('fs', 'tp'), may hold values from -0.125 to 0.125
- value_first: float32 [128, 2048], P('fs', 'tp'), may hold values from -4 to 4
- value_second: float32 [128, 2048], P('fs', 'tp'), may hold values from 0.01 to 0.2
- mixed_heads: bfloat16 [8192, 1024], P('fs', 'tp'), may hold values from -6 to 6
- output_cotangent: bfloat16 [8192, 2048], P('fs', 'tp'), may hold values from -50 to 50
- output_factor: bfloat16 [1024, 128], replicated, may hold values from -10 to 10
- output_master: float32 [1024, 2048], P('fs', 'tp'), may hold values from -0.1875 to 0.1875
- output_first: float32 [128, 2048], P('fs', 'tp'), may hold values from -4 to 4
- output_second: float32 [128, 2048], P('fs', 'tp'), may hold values from 0.01 to 0.2
Outputs:
- value_step: float32 [512, 2048], P('fs', 'tp')
- value_new_master: float32 [512, 2048], P('fs', 'tp')
- value_copy: bfloat16 [512, 2048], P(None, 'tp')
- value_first_new: float32 [128, 2048], P('fs', 'tp')
- value_second_new: float32 [128, 2048], P('fs', 'tp')
- output_step: float32 [1024, 2048], P('fs', 'tp')
- output_new_master: float32 [1024, 2048], P('fs', 'tp')
- output_copy: bfloat16 [1024, 2048], P(None, 'tp')
- output_first_new: float32 [128, 2048], P('fs', 'tp')
- output_second_new: float32 [128, 2048], P('fs', 'tp')
The draws below stay inside these ranges and needn't reach their ends.
All inputs are finite; a program needn't handle non-finite values.
Results may differ from the reference program's by a relative error of at most 0.001.
Values may be sent and summed in bfloat16 or wider, within the bound.
A program may use at most 64 MiB of HBM per device.

```python
import math
import jax
import jax.numpy as jnp
from jax import lax

D = 2048
RANK = 128
HW = 1024
VW = 512
TOKENS = 8192


def column_scaled(key, rows, cols):
    key_rough, key_own = jax.random.split(key, 2)
    ramp = 10.0 ** (jnp.arange(cols, dtype=jnp.float32) / (cols - 1))
    rough = jnp.exp(jax.random.uniform(key_rough, (cols,), jnp.float32, -0.35, 0.35))
    base = jnp.clip(jax.random.normal(key_own, (rows, cols), jnp.float32), -3.5, 3.5)
    return base * ramp[None, :] * rough[None, :]


def draw_value_input(key, part):
    return column_scaled(jax.random.fold_in(key, 11), TOKENS, D).astype(jnp.bfloat16)


def draw_output_cotangent(key, part):
    return column_scaled(jax.random.fold_in(key, 12), TOKENS, D).astype(jnp.bfloat16)


def draw_value_factor(key, part):
    return (column_scaled(jax.random.fold_in(key, 13), VW, RANK) * VW ** (-0.5)).astype(jnp.bfloat16)


def draw_output_factor(key, part):
    return (column_scaled(jax.random.fold_in(key, 14), HW, RANK) * HW ** (-0.5)).astype(jnp.bfloat16)


def level_of(rng, dims, shards, least, largest):
    gain = 1.0
    for position, parts in shards:
        draws = jax.random.uniform(jax.random.fold_in(jax.random.fold_in(rng, 6), position), (parts,), jnp.float32, least / len(shards), largest / len(shards))
        gain = gain * jnp.repeat(jnp.exp(draws), dims[position] // parts).reshape((-1,) + (1,) * (len(dims) - 1 - position))
    return gain


def scatter_about(own_key, dims, scale, bound, cuts=(), kind=jnp.bfloat16):
    result = jax.random.normal(own_key, dims, jnp.float32) * scale
    if len(cuts) > 0:
        result = level_of(own_key, dims, cuts, -0.22, 0.18) * result
    return jnp.clip(result, min=-bound, max=bound).astype(kind)


def setup_inputs(seed: int = 0) -> dict:
    splits = jax.random.split(jax.random.key(seed), 13)
    value_input = draw_value_input(jax.random.fold_in(splits[12], 71), 0)
    value_cotangent = scatter_about(splits[1], (TOKENS, VW), 1.0, 6.0, ((0, 4),))
    value_factor = draw_value_factor(jax.random.fold_in(splits[12], 71), 0)
    value_master = scatter_about(splits[3], (VW, D), D ** -0.5, 0.125, ((0, 4), (1, 8)), jnp.float32)
    value_first = scatter_about(splits[4], (RANK, D), 0.3, 4.0, ((0, 4), (1, 8)), jnp.float32)
    value_second = jnp.clip(jnp.exp(math.log(0.2) - 2.9957323 * jax.random.uniform(splits[5], (RANK, D), jnp.float32) ** level_of(splits[5], (RANK, D), ((0, 4), (1, 8)), -0.2, 0.2)), 0.01, 0.2)
    mixed_heads = scatter_about(splits[6], (TOKENS, HW), 1.0, 6.0, ((0, 4), (1, 8)))
    output_cotangent = draw_output_cotangent(jax.random.fold_in(splits[12], 71), 0)
    output_factor = draw_output_factor(jax.random.fold_in(splits[12], 71), 0)
    output_master = scatter_about(splits[9], (HW, D), HW ** -0.5, 0.1875, ((0, 4), (1, 8)), jnp.float32)
    output_first = scatter_about(splits[10], (RANK, D), 0.3, 4.0, ((0, 4), (1, 8)), jnp.float32)
    output_second = jnp.clip(jnp.exp(math.log(0.2) - 2.9957323 * jax.random.uniform(splits[11], (RANK, D), jnp.float32) ** level_of(splits[11], (RANK, D), ((0, 4), (1, 8)), -0.2, 0.2)), 0.01, 0.2)
    return {"value_input": value_input, "value_cotangent": value_cotangent, "value_factor": value_factor, "value_master": value_master, "value_first": value_first, "value_second": value_second, "mixed_heads": mixed_heads, "output_cotangent": output_cotangent, "output_factor": output_factor, "output_master": output_master, "output_first": output_first, "output_second": output_second}


highest = lax.Precision.HIGHEST

def adam_part(projected, first, second, factor, master):
    scale = lax.rsqrt(jnp.mean(projected * projected) + 1e-06)
    scaled = scale * projected
    first_new = 0.9 * first + 0.1 * scaled
    second_new = 0.95 * second + 0.05 * scaled * scaled
    direction = first_new / (jnp.sqrt(second_new) + 1e-08)
    step = jnp.dot(factor.astype(jnp.float32), direction, precision=highest, preferred_element_type=jnp.float32)
    new_master = master - 0.002 * step
    return (step, new_master, new_master.astype(jnp.bfloat16), first_new, second_new)

def reference(value_input, value_cotangent, value_factor, value_master, value_first, value_second, mixed_heads, output_cotangent, output_factor, output_master, output_first, output_second):
    value_image = jnp.dot(value_cotangent.astype(jnp.float32), value_factor.astype(jnp.float32), precision=highest, preferred_element_type=jnp.float32)
    value_projected = jnp.dot(value_image.T, value_input.astype(jnp.float32), precision=highest, preferred_element_type=jnp.float32)
    output_image = jnp.dot(mixed_heads.astype(jnp.float32), output_factor.astype(jnp.float32), precision=highest, preferred_element_type=jnp.float32)
    output_projected = jnp.dot(output_image.T, output_cotangent.astype(jnp.float32), precision=highest, preferred_element_type=jnp.float32)
    value_out = adam_part(value_projected, value_first, value_second, value_factor, value_master)
    output_out = adam_part(output_projected, output_first, output_second, output_factor, output_master)
    return (value_out[0], value_out[1], value_out[2], value_out[3], value_out[4], output_out[0], output_out[1], output_out[2], output_out[3], output_out[4])
```

```python
import functools

import jax
import jax.numpy as jnp
from jax import lax
from jax.experimental import pallas as pl
from jax.experimental.pallas import tpu as pltpu
from jax.sharding import PartitionSpec as P

MESH = pl.DeviceIdType.MESH
ANY = pl.BlockSpec(memory_space=pl.ANY)
VMEM = pl.BlockSpec(memory_space=pltpu.VMEM)
BF16 = jnp.bfloat16
F32 = jnp.float32


def split(wide, axis):
    high = wide.astype(BF16)
    low = (wide - high.astype(F32)).astype(BF16)
    return jnp.concatenate([high, low], axis=axis)


def gather_kernel(
    fs, tp, pair,
    vin, vcot, vfac, vmas, vm1, vm2, heads, ocot, ofac, omas, om1, om2,
    v_all, o_all, v1_all, v2_all, o1_all, o2_all, vm_all, om_all, totals,
    vin_v, vcot_v, heads_v, ocot_v, v1_v, v2_v, o1_v, o2_v, vm_v, om_v,
    heads_in, images, partial, partial_in, band_v, first_sums, second_sums,
    load_sem, own_sem, put_sem, heads_send, heads_recv, image_send, image_recv, relay_send,
    rs_send, rs_recv, all_send, all_recv, s1_send, s1_recv, s2_send, s2_recv, pre_send, pre_recv,
):
    f = lax.axis_index("fs")
    t = lax.axis_index("tp")
    rank = vfac.shape[1]
    band = rank // fs
    tokens, width = heads.shape
    block = tokens // tp
    columns = vin.shape[1]

    def fs_peer(j):
        return lax.rem(f + j, fs)

    def tp_peer(j):
        return lax.rem(t + j, tp)

    sources = (heads, om1, om2, vm1, vm2, vcot, vin, omas, vmas, ocot)
    places = (heads_v, o1_v, o2_v, v1_v, v2_v, vcot_v, vin_v, om_v, vm_v, ocot_v)
    loads = [
        pltpu.make_async_copy(a, b, load_sem.at[i]) for i, (a, b) in enumerate(zip(sources, places))
    ]
    for load in loads:
        load.start()

    barrier = pltpu.get_barrier_semaphore()
    for j in range(1, tp):
        pl.semaphore_signal(barrier, inc=1, device_id={"tp": tp_peer(j)}, device_id_type=MESH)
    for j in range(1, fs):
        pl.semaphore_signal(barrier, inc=1, device_id={"fs": fs_peer(j)}, device_id_type=MESH)
    pl.semaphore_wait(barrier, tp + fs - 2)

    sent = []

    def send(src, dst, send_sem, recv_sem, where):
        copy = pltpu.make_async_remote_copy(
            src_ref=src, dst_ref=dst, send_sem=send_sem, recv_sem=recv_sem,
            device_id=where, device_id_type=MESH,
        )
        copy.start()
        sent.append(copy)

    def landed(dst, send_sem, recv_sem, where):
        pltpu.make_async_remote_copy(
            src_ref=dst, dst_ref=dst, send_sem=send_sem, recv_sem=recv_sem,
            device_id=where, device_id_type=MESH,
        ).wait_recv()

    loads[0].wait()
    for j in range(1, tp):
        d = tp_peer(j)
        send(
            heads_v.at[pl.ds(pl.multiple_of(d * block, block), block)], heads_in.at[t],
            heads_send.at[j], heads_recv.at[t], {"tp": d},
        )
    own_heads = pltpu.make_async_copy(
        heads_v.at[pl.ds(pl.multiple_of(t * block, block), block)], heads_in.at[t], own_sem
    )
    own_heads.start()

    puts = []

    def prefetch(i, load, local, whole):
        load.wait()
        rows = local.shape[0]
        here = whole.at[pl.ds(pl.multiple_of(f * rows, rows), rows)]
        for j in range(1, fs):
            d = fs_peer(j)
            send(local, here, pre_send.at[i, j], pre_recv.at[i, f], {"fs": d})
        put = pltpu.make_async_copy(local, here, put_sem.at[i])
        put.start()
        puts.append(put)

    prefetch(0, loads[1], o1_v, o1_all)
    prefetch(1, loads[2], o2_v, o2_all)
    prefetch(2, loads[3], v1_v, v1_all)
    prefetch(3, loads[4], v2_v, v2_all)

    loads[5].wait()
    loads[6].wait()
    total = jnp.zeros((2 * rank, columns), F32)
    step = 256 if tokens % 256 == 0 else tokens
    for i in range(tokens // step):
        rows = pl.ds(i * step, step)
        image = jnp.dot(vcot_v[rows, :], vfac[...], preferred_element_type=F32)
        total = total + lax.dot_general(
            split(image, 1), vin_v[rows, :], (((0,), (0,)), ((), ())), preferred_element_type=F32
        )

    def scatter(k, total):
        partial[k] = (total[:rank] + total[rank:]).reshape(fs, band, columns)
        for j in range(1, fs):
            d = fs_peer(j)
            send(partial.at[k, d], partial_in.at[k, f], rs_send.at[k, j], rs_recv.at[k, f], {"fs": d})

    def reduce(k, whole):
        mine = partial[k, f]
        for j in range(1, fs):
            d = fs_peer(j)
            landed(partial_in.at[k, d], rs_send.at[k, j], rs_recv.at[k, d], {"fs": d})
            mine = mine + partial_in[k, d]
        band_v[k] = mine
        first_sums[k, f] = jnp.full((8, 128), jnp.sum(mine * mine), F32)
        for j in range(1, fs):
            d = fs_peer(j)
            send(first_sums.at[k, f], first_sums.at[k, f], s1_send.at[k, j], s1_recv.at[k, f], {"fs": d})
        for j in range(1, fs):
            d = fs_peer(j)
            send(band_v.at[k], whole.at[f], all_send.at[k, j], all_recv.at[k, f], {"fs": d})
        put = pltpu.make_async_copy(band_v.at[k], whole.at[f], put_sem.at[6 + k])
        put.start()
        puts.append(put)

    def sums_on(k):
        mine = first_sums[k, f]
        for j in range(1, fs):
            d = fs_peer(j)
            landed(first_sums.at[k, d], s1_send.at[k, j], s1_recv.at[k, d], {"fs": d})
            mine = mine + first_sums[k, d]
        second_sums[k, t] = mine
        for j in range(1, tp):
            d = tp_peer(j)
            send(second_sums.at[k, t], second_sums.at[k, t], s2_send.at[k, j], s2_recv.at[k, t], {"tp": d})

    def sums_end(k):
        mine = second_sums[k, t]
        for j in range(1, tp):
            d = tp_peer(j)
            landed(second_sums.at[k, d], s2_send.at[k, j], s2_recv.at[k, d], {"tp": d})
            mine = mine + second_sums[k, d]
        totals[k] = mine

    scatter(0, total)
    prefetch(4, loads[7], om_v, om_all)
    prefetch(5, loads[8], vm_v, vm_all)

    own_heads.wait()

    def image_term(s):
        return jnp.dot(
            heads_in[s], ofac[pl.ds(pl.multiple_of(s * width, width), width), :],
            preferred_element_type=F32,
        )

    image = image_term(t)
    for j in range(1, tp):
        d = tp_peer(j)
        landed(heads_in.at[d], heads_send.at[j], heads_recv.at[d], {"tp": d})
        image = image + image_term(d)
    images[t] = image.T

    chip = t // pair
    core = t % pair
    chips = tp // pair

    def give(d, j):
        send(images.at[t], images.at[t], image_send.at[j], image_recv.at[t], {"tp": d})

    for j in range(1, chips):
        give(lax.rem(chip + j, chips) * pair + core, j - 1)
    for j in range(1, pair):
        give(chip * pair + lax.rem(core + j, pair), chips - 2 + j)

    loads[9].wait()

    def term(s):
        return jnp.dot(
            split(images[s], 0), ocot_v[pl.ds(pl.multiple_of(s * block, block), block), :],
            preferred_element_type=F32,
        )

    total = term(t)
    reduce(0, v_all)

    def arrived(s):
        landed(images.at[s], image_send.at[0], image_recv.at[s], {"tp": s})

    for j in range(1, pair):
        s = chip * pair + lax.rem(core + j, pair)
        arrived(s)
        total = total + term(s)
    for j in range(1, chips):
        s = lax.rem(chip + j, chips) * pair + core
        arrived(s)
        for i in range(1, pair):
            send(
                images.at[s], images.at[s], relay_send.at[(j - 1) * (pair - 1) + i - 1],
                image_recv.at[s], {"tp": chip * pair + lax.rem(core + i, pair)},
            )
        total = total + term(s)
    for j in range(1, chips):
        for i in range(1, pair):
            s = lax.rem(chip + j, chips) * pair + lax.rem(core + i, pair)
            arrived(s)
            total = total + term(s)

    scatter(1, total)
    sums_on(0)
    reduce(1, o_all)
    sums_on(1)
    sums_end(0)
    sums_end(1)

    for k, whole in ((0, v_all), (1, o_all)):
        for j in range(1, fs):
            d = fs_peer(j)
            landed(whole.at[d], all_send.at[k, j], all_recv.at[k, d], {"fs": d})
    for i, (local, whole) in enumerate(
        ((o1_v, o1_all), (o2_v, o2_all), (v1_v, v1_all), (v2_v, v2_all), (om_v, om_all), (vm_v, vm_all))
    ):
        rows = local.shape[0]
        for j in range(1, fs):
            d = fs_peer(j)
            there = whole.at[pl.ds(pl.multiple_of(d * rows, rows), rows)]
            landed(there, pre_send.at[i, j], pre_recv.at[i, d], {"fs": d})
    for copy in sent:
        copy.wait_send()
    for put in puts:
        put.wait()


def finish_kernel(
    fs, tp,
    v_all, o_all, v1_all, v2_all, o1_all, o2_all, vm_all, om_all, totals, vfac, ofac,
    v_step, v_new, v_copy, v_first, v_second, o_step, o_new, o_copy, o_first, o_second,
):
    f = lax.axis_index("fs")

    def one(k, proj, first, second, master, factor, step_out, new_out, copy_out, first_out, second_out):
        rank, columns = proj.shape
        scale = lax.rsqrt(totals[k, 0:1, 0:1] / (rank * columns * tp) + 1e-06)

        def moments(rows):
            scaled = scale * proj[rows, :]
            first_new = 0.9 * first[rows, :] + 0.1 * scaled
            second_new = 0.95 * second[rows, :] + 0.05 * scaled * scaled
            return first_new, second_new

        band = rank // fs
        first_own, second_own = moments(pl.ds(pl.multiple_of(f * band, band), band))
        first_out[...] = first_own
        second_out[...] = second_own
        first_new, second_new = moments(pl.ds(0, rank))
        direction = split(first_new / (jnp.sqrt(second_new) + 1e-08), 0)

        def step_of(rows):
            left = factor[rows, :]
            return jnp.dot(
                jnp.concatenate([left, left], axis=1), direction, preferred_element_type=F32
            )

        count = step_out.shape[0]
        own = pl.ds(pl.multiple_of(f * count, count), count)
        step = step_of(own)
        step_out[...] = step
        new_out[...] = master[own, :] - 0.002 * step
        for i in range(fs):
            rows = pl.ds(i * count, count)
            copy_out[rows, :] = (master[rows, :] - 0.002 * step_of(rows)).astype(BF16)

    one(0, v_all, v1_all, v2_all, vm_all, vfac, v_step, v_new, v_copy, v_first, v_second)
    one(1, o_all, o1_all, o2_all, om_all, ofac, o_step, o_new, o_copy, o_first, o_second)


def on_device(vin, vcot, vfac, vmas, vm1, vm2, heads, ocot, ofac, omas, om1, om2):
    fs = lax.axis_size("fs")
    tp = lax.axis_size("tp")
    pair = 2 if tp % 2 == 0 else 1
    rank = vfac.shape[1]
    band = rank // fs
    columns = vin.shape[1]
    tokens, width = heads.shape
    block = tokens // tp

    def like(array):
        return pltpu.VMEM(array.shape, array.dtype)

    def shape(*dims):
        return jax.ShapeDtypeStruct(dims, F32)

    dma = pltpu.SemaphoreType.DMA
    gathered = pl.pallas_call(
        functools.partial(gather_kernel, fs, tp, pair),
        out_shape=(
            shape(fs, band, columns), shape(fs, band, columns),
            shape(rank, columns), shape(rank, columns), shape(rank, columns), shape(rank, columns),
            shape(fs * vmas.shape[0], columns), shape(fs * omas.shape[0], columns),
            shape(2, 8, 128),
        ),
        in_specs=[ANY, ANY, VMEM, ANY, ANY, ANY, ANY, ANY, VMEM, ANY, ANY, ANY],
        out_specs=(ANY,) * 8 + (VMEM,),
        scratch_shapes=[
            like(vin), like(vcot), like(heads), like(ocot), like(vm1), like(vm2), like(om1), like(om2),
            like(vmas), like(omas),
            pltpu.VMEM((tp, block, width), BF16),
            pltpu.VMEM((tp, rank, block), F32),
            pltpu.VMEM((2, fs, band, columns), F32),
            pltpu.VMEM((2, fs, band, columns), F32),
            pltpu.VMEM((2, band, columns), F32),
            pltpu.VMEM((2, fs, 8, 128), F32),
            pltpu.VMEM((2, tp, 8, 128), F32),
            dma((10,)), dma, dma((8,)), dma((tp,)), dma((tp,)), dma((tp,)), dma((tp,)), dma((tp,)),
            dma((2, fs)), dma((2, fs)), dma((2, fs)), dma((2, fs)), dma((2, fs)), dma((2, fs)),
            dma((2, tp)), dma((2, tp)), dma((6, fs)), dma((6, fs)),
        ],
        compiler_params=pltpu.CompilerParams(
            collective_id=0, has_side_effects=True, vmem_limit_bytes=40 * 1024 * 1024
        ),
    )(vin, vcot, vfac, vmas, vm1, vm2, heads, ocot, ofac, omas, om1, om2)
    v_all, o_all, v1_all, v2_all, o1_all, o2_all, vm_all, om_all, totals = gathered
    v_all = v_all.reshape(rank, columns)
    o_all = o_all.reshape(rank, columns)

    def out(array, rows, kind=F32):
        return jax.ShapeDtypeStruct((rows, columns), kind)

    return pl.pallas_call(
        functools.partial(finish_kernel, fs, tp),
        out_shape=(
            out(vmas, vmas.shape[0]), out(vmas, vmas.shape[0]), out(vmas, fs * vmas.shape[0], BF16),
            out(vm1, band), out(vm1, band),
            out(omas, omas.shape[0]), out(omas, omas.shape[0]), out(omas, fs * omas.shape[0], BF16),
            out(om1, band), out(om1, band),
        ),
        in_specs=[VMEM] * 11,
        out_specs=(VMEM,) * 10,
        compiler_params=pltpu.CompilerParams(vmem_limit_bytes=40 * 1024 * 1024),
    )(v_all, o_all, v1_all, v2_all, o1_all, o2_all, vm_all, om_all, totals, vfac, ofac)


def solution(mesh):
    both = P("fs", "tp")
    in_specs = (both, P("fs", None), P(), both, both, both, both, both, P(), both, both, both)
    out_specs = (
        both, both, P(None, "tp"), both, both, both, both, P(None, "tp"), both, both,
    )
    return jax.shard_map(
        on_device, mesh=mesh, in_specs=in_specs, out_specs=out_specs, check_vma=False
    )
```

```python
import functools

import jax
import jax.numpy as jnp
from jax import lax
from jax.experimental import pallas as pl
from jax.experimental.pallas import tpu as pltpu
from jax.sharding import PartitionSpec as P

MESH = pl.DeviceIdType.MESH
ANY = pl.BlockSpec(memory_space=pl.ANY)
HBM = pl.BlockSpec(memory_space=pltpu.HBM)
VMEM = pl.BlockSpec(memory_space=pltpu.VMEM)
BF16 = jnp.bfloat16
F32 = jnp.float32


def split(wide, axis):
    high = wide.astype(BF16)
    low = (wide - high.astype(F32)).astype(BF16)
    return jnp.concatenate([high, low], axis=axis)


def gather_kernel(
    fs, tp, pair,
    vin, vcot, vfac, vmas, vm1, vm2, heads, ocot, ofac, omas, om1, om2,
    v_all, o_all, v1_all, v2_all, o1_all, o2_all, vm_all, om_all, totals,
    vfac_v, ofac_v, vin_v, vcot_v, heads_v, ocot_v, v1_v, v2_v, o1_v, o2_v, vm_v, om_v,
    heads_in, images, partial, partial_in, band_v, first_sums, second_sums,
    load_sem, own_sem, put_sem, heads_send, heads_recv, image_send, image_recv, relay_send,
    rs_send, rs_recv, all_send, all_recv, s1_send, s1_recv, s2_send, s2_recv, pre_send, pre_recv,
):
    f = lax.axis_index("fs")
    t = lax.axis_index("tp")
    rank = vfac.shape[1]
    band = rank // fs
    tokens, width = heads.shape
    block = tokens // tp
    columns = vin.shape[1]

    def fs_peer(j):
        return lax.rem(f + j, fs)

    def tp_peer(j):
        return lax.rem(t + j, tp)

    sources = (heads, om1, om2, vm1, vm2, vcot, vin, omas, vmas, ocot, vfac, ofac)
    places = (heads_v, o1_v, o2_v, v1_v, v2_v, vcot_v, vin_v, om_v, vm_v, ocot_v, vfac_v, ofac_v)
    loads = [
        pltpu.make_async_copy(a, b, load_sem.at[i]) for i, (a, b) in enumerate(zip(sources, places))
    ]
    for load in loads:
        load.start()

    barrier = pltpu.get_barrier_semaphore()
    for j in range(1, tp):
        pl.semaphore_signal(barrier, inc=1, device_id={"tp": tp_peer(j)}, device_id_type=MESH)
    for j in range(1, fs):
        pl.semaphore_signal(barrier, inc=1, device_id={"fs": fs_peer(j)}, device_id_type=MESH)
    pl.semaphore_wait(barrier, tp + fs - 2)

    sent = []

    def send(src, dst, send_sem, recv_sem, where):
        copy = pltpu.make_async_remote_copy(
            src_ref=src, dst_ref=dst, send_sem=send_sem, recv_sem=recv_sem,
            device_id=where, device_id_type=MESH,
        )
        copy.start()
        sent.append(copy)

    def landed(dst, send_sem, recv_sem, where):
        pltpu.make_async_remote_copy(
            src_ref=dst, dst_ref=dst, send_sem=send_sem, recv_sem=recv_sem,
            device_id=where, device_id_type=MESH,
        ).wait_recv()

    loads[0].wait()
    for j in range(1, tp):
        d = tp_peer(j)
        send(
            heads_v.at[pl.ds(pl.multiple_of(d * block, block), block)], heads_in.at[t],
            heads_send.at[j], heads_recv.at[t], {"tp": d},
        )
    own_heads = pltpu.make_async_copy(
        heads_v.at[pl.ds(pl.multiple_of(t * block, block), block)], heads_in.at[t], own_sem
    )
    own_heads.start()

    puts = []

    def prefetch(i, load, local, whole):
        load.wait()
        rows = local.shape[0]
        here = whole.at[pl.ds(pl.multiple_of(f * rows, rows), rows)]
        for j in range(1, fs):
            d = fs_peer(j)
            send(local, here, pre_send.at[i, j], pre_recv.at[i, f], {"fs": d})
        put = pltpu.make_async_copy(local, here, put_sem.at[i])
        put.start()
        puts.append(put)

    prefetch(0, loads[1], o1_v, o1_all)
    prefetch(1, loads[2], o2_v, o2_all)
    prefetch(2, loads[3], v1_v, v1_all)
    prefetch(3, loads[4], v2_v, v2_all)

    loads[5].wait()
    loads[6].wait()
    loads[10].wait()
    total = jnp.zeros((2 * rank, columns), F32)
    step = 256 if tokens % 256 == 0 else tokens
    for i in range(tokens // step):
        rows = pl.ds(i * step, step)
        image = jnp.dot(vcot_v[rows, :], vfac_v[...], preferred_element_type=F32)
        total = total + lax.dot_general(
            split(image, 1), vin_v[rows, :], (((0,), (0,)), ((), ())), preferred_element_type=F32
        )

    def scatter(k, total):
        partial[k] = (total[:rank] + total[rank:]).reshape(fs, band, columns)
        for j in range(1, fs):
            d = fs_peer(j)
            send(partial.at[k, d], partial_in.at[k, f], rs_send.at[k, j], rs_recv.at[k, f], {"fs": d})

    def reduce(k, whole):
        mine = partial[k, f]
        for j in range(1, fs):
            d = fs_peer(j)
            landed(partial_in.at[k, d], rs_send.at[k, j], rs_recv.at[k, d], {"fs": d})
            mine = mine + partial_in[k, d]
        band_v[k] = mine
        first_sums[k, f] = jnp.full((8, 128), jnp.sum(mine * mine), F32)
        for j in range(1, fs):
            d = fs_peer(j)
            send(first_sums.at[k, f], first_sums.at[k, f], s1_send.at[k, j], s1_recv.at[k, f], {"fs": d})
        for j in range(1, fs):
            d = fs_peer(j)
            send(band_v.at[k], whole.at[f], all_send.at[k, j], all_recv.at[k, f], {"fs": d})
        put = pltpu.make_async_copy(band_v.at[k], whole.at[f], put_sem.at[6 + k])
        put.start()
        puts.append(put)

    def sums_on(k):
        mine = first_sums[k, f]
        for j in range(1, fs):
            d = fs_peer(j)
            landed(first_sums.at[k, d], s1_send.at[k, j], s1_recv.at[k, d], {"fs": d})
            mine = mine + first_sums[k, d]
        second_sums[k, t] = mine
        for j in range(1, tp):
            d = tp_peer(j)
            send(second_sums.at[k, t], second_sums.at[k, t], s2_send.at[k, j], s2_recv.at[k, t], {"tp": d})

    def sums_end(k):
        mine = second_sums[k, t]
        for j in range(1, tp):
            d = tp_peer(j)
            landed(second_sums.at[k, d], s2_send.at[k, j], s2_recv.at[k, d], {"tp": d})
            mine = mine + second_sums[k, d]
        totals[k] = mine

    scatter(0, total)
    prefetch(4, loads[7], om_v, om_all)
    prefetch(5, loads[8], vm_v, vm_all)

    own_heads.wait()
    loads[11].wait()

    def image_term(s):
        return jnp.dot(
            heads_in[s], ofac_v[pl.ds(pl.multiple_of(s * width, width), width), :],
            preferred_element_type=F32,
        )

    image = image_term(t)
    for j in range(1, tp):
        d = tp_peer(j)
        landed(heads_in.at[d], heads_send.at[j], heads_recv.at[d], {"tp": d})
        image = image + image_term(d)
    images[t] = image.T

    chip = t // pair
    core = t % pair
    chips = tp // pair

    def give(d, j):
        send(images.at[t], images.at[t], image_send.at[j], image_recv.at[t], {"tp": d})

    for j in range(1, chips):
        give(lax.rem(chip + j, chips) * pair + core, j - 1)
    for j in range(1, pair):
        give(chip * pair + lax.rem(core + j, pair), chips - 2 + j)

    loads[9].wait()

    def term(s):
        return jnp.dot(
            split(images[s], 0), ocot_v[pl.ds(pl.multiple_of(s * block, block), block), :],
            preferred_element_type=F32,
        )

    total = term(t)
    reduce(0, v_all)

    def arrived(s):
        landed(images.at[s], image_send.at[0], image_recv.at[s], {"tp": s})

    for j in range(1, pair):
        s = chip * pair + lax.rem(core + j, pair)
        arrived(s)
        total = total + term(s)
    for j in range(1, chips):
        s = lax.rem(chip + j, chips) * pair + core
        arrived(s)
        for i in range(1, pair):
            send(
                images.at[s], images.at[s], relay_send.at[(j - 1) * (pair - 1) + i - 1],
                image_recv.at[s], {"tp": chip * pair + lax.rem(core + i, pair)},
            )
        total = total + term(s)
    for j in range(1, chips):
        for i in range(1, pair):
            s = lax.rem(chip + j, chips) * pair + lax.rem(core + i, pair)
            arrived(s)
            total = total + term(s)

    scatter(1, total)
    sums_on(0)
    reduce(1, o_all)
    sums_on(1)
    sums_end(0)
    sums_end(1)

    for k, whole in ((0, v_all), (1, o_all)):
        for j in range(1, fs):
            d = fs_peer(j)
            landed(whole.at[d], all_send.at[k, j], all_recv.at[k, d], {"fs": d})
    for i, (local, whole) in enumerate(
        ((o1_v, o1_all), (o2_v, o2_all), (v1_v, v1_all), (v2_v, v2_all), (om_v, om_all), (vm_v, vm_all))
    ):
        rows = local.shape[0]
        for j in range(1, fs):
            d = fs_peer(j)
            there = whole.at[pl.ds(pl.multiple_of(d * rows, rows), rows)]
            landed(there, pre_send.at[i, j], pre_recv.at[i, d], {"fs": d})
    for copy in sent:
        copy.wait_send()
    for put in puts:
        put.wait()


def finish_kernel(
    fs, tp,
    v_all, o_all, v1_all, v2_all, o1_all, o2_all, vm_all, om_all, totals, vfac, ofac,
    v_step, v_new, v_copy, v_first, v_second, o_step, o_new, o_copy, o_first, o_second,
):
    f = lax.axis_index("fs")

    def one(k, proj, first, second, master, factor, step_out, new_out, copy_out, first_out, second_out):
        rank, columns = proj.shape
        scale = lax.rsqrt(totals[k, 0:1, 0:1] / (rank * columns * tp) + 1e-06)

        def moments(rows):
            scaled = scale * proj[rows, :]
            first_new = 0.9 * first[rows, :] + 0.1 * scaled
            second_new = 0.95 * second[rows, :] + 0.05 * scaled * scaled
            return first_new, second_new

        band = rank // fs
        first_own, second_own = moments(pl.ds(pl.multiple_of(f * band, band), band))
        first_out[...] = first_own
        second_out[...] = second_own
        first_new, second_new = moments(pl.ds(0, rank))
        direction = split(first_new / (jnp.sqrt(second_new) + 1e-08), 0)

        def step_of(rows):
            left = factor[rows, :]
            return jnp.dot(
                jnp.concatenate([left, left], axis=1), direction, preferred_element_type=F32
            )

        count = step_out.shape[0]
        own = pl.ds(pl.multiple_of(f * count, count), count)
        step = step_of(own)
        step_out[...] = step
        new_out[...] = master[own, :] - 0.002 * step
        for i in range(fs):
            rows = pl.ds(i * count, count)
            copy_out[rows, :] = (master[rows, :] - 0.002 * step_of(rows)).astype(BF16)

    one(0, v_all, v1_all, v2_all, vm_all, vfac, v_step, v_new, v_copy, v_first, v_second)
    one(1, o_all, o1_all, o2_all, om_all, ofac, o_step, o_new, o_copy, o_first, o_second)


def on_device(vin, vcot, vfac, vmas, vm1, vm2, heads, ocot, ofac, omas, om1, om2):
    fs = lax.axis_size("fs")
    tp = lax.axis_size("tp")
    pair = 2 if tp % 2 == 0 else 1
    rank = vfac.shape[1]
    band = rank // fs
    columns = vin.shape[1]
    tokens, width = heads.shape
    block = tokens // tp

    def like(array):
        return pltpu.VMEM(array.shape, array.dtype)

    def shape(*dims):
        return jax.ShapeDtypeStruct(dims, F32)

    dma = pltpu.SemaphoreType.DMA
    gathered = pl.pallas_call(
        functools.partial(gather_kernel, fs, tp, pair),
        out_shape=(
            shape(fs, band, columns), shape(fs, band, columns),
            shape(rank, columns), shape(rank, columns), shape(rank, columns), shape(rank, columns),
            shape(fs * vmas.shape[0], columns), shape(fs * omas.shape[0], columns),
            shape(2, 8, 128),
        ),
        in_specs=[HBM] * 12,
        out_specs=(ANY,) * 8 + (VMEM,),
        scratch_shapes=[
            like(vfac), like(ofac), like(vin), like(vcot), like(heads), like(ocot), like(vm1), like(vm2), like(om1), like(om2),
            like(vmas), like(omas),
            pltpu.VMEM((tp, block, width), BF16),
            pltpu.VMEM((tp, rank, block), F32),
            pltpu.VMEM((2, fs, band, columns), F32),
            pltpu.VMEM((2, fs, band, columns), F32),
            pltpu.VMEM((2, band, columns), F32),
            pltpu.VMEM((2, fs, 8, 128), F32),
            pltpu.VMEM((2, tp, 8, 128), F32),
            dma((12,)), dma, dma((8,)), dma((tp,)), dma((tp,)), dma((tp,)), dma((tp,)), dma((tp,)),
            dma((2, fs)), dma((2, fs)), dma((2, fs)), dma((2, fs)), dma((2, fs)), dma((2, fs)),
            dma((2, tp)), dma((2, tp)), dma((6, fs)), dma((6, fs)),
        ],
        compiler_params=pltpu.CompilerParams(
            collective_id=0, has_side_effects=True, vmem_limit_bytes=60 * 1024 * 1024
        ),
    )(vin, vcot, vfac, vmas, vm1, vm2, heads, ocot, ofac, omas, om1, om2)
    v_all, o_all, v1_all, v2_all, o1_all, o2_all, vm_all, om_all, totals = gathered
    v_all = v_all.reshape(rank, columns)
    o_all = o_all.reshape(rank, columns)

    def out(array, rows, kind=F32):
        return jax.ShapeDtypeStruct((rows, columns), kind)

    return pl.pallas_call(
        functools.partial(finish_kernel, fs, tp),
        out_shape=(
            out(vmas, vmas.shape[0]), out(vmas, vmas.shape[0]), out(vmas, fs * vmas.shape[0], BF16),
            out(vm1, band), out(vm1, band),
            out(omas, omas.shape[0]), out(omas, omas.shape[0]), out(omas, fs * omas.shape[0], BF16),
            out(om1, band), out(om1, band),
        ),
        in_specs=[VMEM] * 11,
        out_specs=(VMEM,) * 10,
        compiler_params=pltpu.CompilerParams(vmem_limit_bytes=60 * 1024 * 1024),
    )(v_all, o_all, v1_all, v2_all, o1_all, o2_all, vm_all, om_all, totals, vfac, ofac)


def solution(mesh):
    both = P("fs", "tp")
    in_specs = (both, P("fs", None), P(), both, both, both, both, both, P(), both, both, both)
    out_specs = (
        both, both, P(None, "tp"), both, both, both, both, P(None, "tp"), both, both,
    )
    return jax.shard_map(
        on_device, mesh=mesh, in_specs=in_specs, out_specs=out_specs, check_vma=False
    )
```
